512 devices in a mesh: grp: 2 (over y), sp: 32 (over z), tp: 8 (over x, core).
Axes of the slice: x: 4, y: 2, z: 32, core: 2. Of those that a mesh axis runs over, the one named last changes fastest.
The devices are a block of a 4x8x32 slice.
Arguments:
- latent: bfloat16 [24576, 2048], P(('grp', 'sp')), parts along dimension 0, may hold values from -6 to 6
- conditioning: bfloat16 [4096], P(('grp', 'sp')), parts along dimension 0, may hold values from -6 to 6
- context: bfloat16 [1024, 2048], P(('grp', 'sp')), parts along dimension 0, may hold values from -6 to 6
- ctx_vector: bfloat16 [2048], P('sp'), may hold values from -6 to 6
- w_shift: bfloat16 [2048, 2048], P('sp', 'tp'), may hold values from -0.25 to 0.25
- w_scale: bfloat16 [2048, 2048], P('sp', 'tp'), may hold values from -0.25 to 0.25
- w_gate: bfloat16 [2048, 2048], P('sp', 'tp'), may hold values from -0.25 to 0.25
- norm_gain: bfloat16 [2048], replicated, may hold values from 0.099609375 to 1.8984375
- w_query: bfloat16 [2048, 1024], P(None, 'tp'), may hold values from -1 to 1
- w_key: bfloat16 [2048, 1024], P(None, 'tp'), may hold values from -1 to 1
- w_value: bfloat16 [2048, 1024], P(None, 'tp'), may hold values from -0.125 to 0.125
- offset_bias: float32 [16, 15, 31], P('tp'), may hold values from 1.5 to 4.5
- w_out: bfloat16 [1024, 2048], P(None, 'tp'), may hold values from -0.75 to 0.75
Outputs:
- mixed_out: bfloat16 [24576, 2048], P(('grp', 'sp'), 'tp'), parts along dimension 0
The draws below stay inside these ranges and needn't reach their ends.
There are 2 independent parts, one for each index of `grp`. The reference program is written for one: setup_inputs(seed, part) draws one part's arguments, and reference() takes and returns one part's arrays. A program takes and returns all parts, laid end to end along the dimension named above; an argument that names none is the same for every part. Nothing has to cross between parts.
All inputs are finite; a program needn't handle non-finite values.
Results may differ from the reference program's by a relative error of at most 0.011.
Values may be sent and summed in bfloat16 or wider, within the bound.
A program may use at most 64 MiB of HBM per device.

```python
import jax
import jax.numpy as jnp
from jax import lax

D = 2048
HEADS = 16
HEAD_DIM = 64
GRID_W = 64
WIN_H = 8
WIN_W = 16
ROWS_DEV = 6
TOKENS = 12288
CTX = 512
WIDTH = 1024
N_SP = 32


def weight_pair(key):
    base_key = jax.random.fold_in(key, 101)
    first_key, second_key = jax.random.split(base_key, 2)
    columns = HEADS * HEAD_DIM
    first = jax.random.normal(first_key, (D, columns), jnp.float32) * D ** (-0.5)
    second = jax.random.normal(second_key, (D, columns), jnp.float32) * D ** (-0.5)
    query_weight = first
    key_weight = second
    return (jnp.clip(query_weight, -1.0, 1.0), jnp.clip(key_weight, -1.0, 1.0))


def draw_w_query(key, part):
    return weight_pair(key)[0].astype(jnp.bfloat16)


def draw_w_key(key, part):
    return weight_pair(key)[1].astype(jnp.bfloat16)


def level_of(key, extent, cuts, smallest, top_value):
    gain, own = 1.0, jax.random.fold_in(key, 6)
    for dim, parts in cuts:
        heights = jnp.exp(jax.random.uniform(jax.random.fold_in(own, dim), (parts,), jnp.float32, smallest / len(cuts), top_value / len(cuts)))
        gain = gain * jnp.repeat(heights, extent[dim] // parts).reshape([-1 if axis == dim else 1 for axis in range(len(extent))])
    return gain


def noise(rng, extent, spread, reach, cuts=(), held_as=jnp.bfloat16):
    loudness = level_of(rng, extent, cuts, -0.22, 0.18) if cuts else 1.0
    values = jax.random.normal(rng, extent, jnp.float32) * spread * loudness
    return jnp.minimum(jnp.maximum(values, -reach), reach).astype(held_as)


def setup_inputs(seed: int = 0, part: int = 0) -> dict:
    streams_of = jax.random.split(jax.random.key(seed), 14)
    part_splits = jax.random.split(jax.random.fold_in(streams_of[13], part), 14)
    latent = noise(part_splits[0], (TOKENS, D), 1.0, 6.0, ((0, 32),))
    conditioning = noise(part_splits[1], (D,), 1.0, 6.0, ((0, 32),))
    context = noise(part_splits[2], (CTX, D), 1.0, 6.0, ((0, 32),))
    ctx_vector = noise(streams_of[3], (D,), 1.0, 6.0, ((0, 32),))
    w_shift = noise(streams_of[4], (D, D), (D // 4) ** -0.5, 0.25, ((0, 32), (1, 8)))
    w_scale = noise(streams_of[5], (D, D), (D // 4) ** -0.5, 0.25, ((0, 32), (1, 8)))
    w_gate = noise(streams_of[6], (D, D), (D // 4) ** -0.5, 0.25, ((0, 32), (1, 8)))
    norm_gain = jnp.clip(1.0 + 0.18 * jax.random.normal(streams_of[7], (D,), jnp.float32), 0.099609375, 1.8984375).astype(jnp.bfloat16)
    w_query = draw_w_query(jax.random.fold_in(streams_of[13], 71), part)
    w_key = draw_w_key(jax.random.fold_in(streams_of[13], 71), part)
    w_value = noise(streams_of[10], (D, WIDTH), D ** -0.5, 0.125, ((1, 8),))
    offset_bias = jnp.clip(1.5 + 3.0 * jax.random.uniform(streams_of[11], (HEADS, 2 * WIN_H - 1, 2 * WIN_W - 1), jnp.float32) ** level_of(streams_of[11], (HEADS, 2 * WIN_H - 1, 2 * WIN_W - 1), ((0, 8),), -0.2, 0.2), 1.5, 4.5)
    w_out = noise(streams_of[12], (WIDTH, D), (WIDTH // 16) ** -0.5, 0.75, ((1, 8),))
    return dict(latent=latent, conditioning=conditioning, context=context, ctx_vector=ctx_vector, w_shift=w_shift, w_scale=w_scale, w_gate=w_gate, norm_gain=norm_gain, w_query=w_query, w_key=w_key, w_value=w_value, offset_bias=offset_bias, w_out=w_out)


EPSILON = 1e-06

def modulated_norm(inputs, norm_gain, shift_vec, scale_vec):
    floats = inputs.astype(jnp.float32)
    inverse = lax.rsqrt(lax.optimization_barrier(jnp.mean(floats * floats, axis=-1, keepdims=True)) + EPSILON)
    return (floats * inverse * norm_gain.astype(jnp.float32) * (1.0 + scale_vec) + shift_vec).astype(jnp.bfloat16)

def project(inputs, weight):
    return jnp.dot(inputs, weight, preferred_element_type=jnp.float32).astype(jnp.bfloat16)

def reference(latent, conditioning, context, ctx_vector, w_shift, w_scale, w_gate, norm_gain, w_query, w_key, w_value, offset_bias, w_out):
    cond_act = jax.nn.silu(conditioning.astype(jnp.float32)).astype(jnp.bfloat16)
    ctx_act = jax.nn.silu(ctx_vector.astype(jnp.float32)).astype(jnp.bfloat16)
    shift_vec = jnp.dot(cond_act, w_shift, preferred_element_type=jnp.float32)
    scale_vec = jnp.dot(cond_act, w_scale, preferred_element_type=jnp.float32)
    gate_vec = jnp.dot(cond_act, w_gate, preferred_element_type=jnp.float32)
    ctx_shift = jnp.dot(ctx_act, w_shift, preferred_element_type=jnp.float32)
    ctx_scale = jnp.dot(ctx_act, w_scale, preferred_element_type=jnp.float32)
    normed = modulated_norm(latent, norm_gain, shift_vec, scale_vec)
    ctx_normed = modulated_norm(context, norm_gain, ctx_shift, ctx_scale)
    queries = project(normed, w_query)
    keys_lat = project(normed, w_key)
    values_lat = project(normed, w_value)
    ctx_keys = project(ctx_normed, w_key).astype(jnp.float32).reshape(-1, HEADS, HEAD_DIM)
    ctx_values = project(ctx_normed, w_value).astype(jnp.float32).reshape(-1, HEADS, HEAD_DIM)
    grid_rows = ROWS_DEV * N_SP
    query_grid = queries.astype(jnp.float32).reshape(grid_rows, GRID_W, HEADS, HEAD_DIM)
    key_grid = keys_lat.astype(jnp.float32).reshape(grid_rows, GRID_W, HEADS, HEAD_DIM)
    value_grid = values_lat.astype(jnp.float32).reshape(grid_rows, GRID_W, HEADS, HEAD_DIM)
    columns = jnp.arange(GRID_W, dtype=jnp.int32)
    col_index = jnp.clip(columns - WIN_W // 2, 0, GRID_W - WIN_W)[:, None] + jnp.arange(WIN_W, dtype=jnp.int32)[None, :]
    col_offset = (col_index - columns[:, None] + WIN_W - 1).astype(jnp.int32)
    scale_qk = HEAD_DIM ** (-0.5)
    bias_table = offset_bias.astype(jnp.float32)

    def one_row(grid_row):
        first_row = jnp.clip(grid_row - WIN_H // 2, 0, grid_rows - WIN_H).astype(jnp.int32)
        key_rows = lax.dynamic_slice_in_dim(key_grid, first_row, WIN_H, 0)
        value_rows = lax.dynamic_slice_in_dim(value_grid, first_row, WIN_H, 0)
        key_window = key_rows[:, col_index]
        value_window = value_rows[:, col_index]
        query_row = lax.dynamic_index_in_dim(query_grid, grid_row, 0, keepdims=False)
        row_offset = (first_row + jnp.arange(WIN_H, dtype=jnp.int32) - grid_row + WIN_H - 1).astype(jnp.int32)
        offset_terms = bias_table[:, row_offset[:, None, None], col_offset[None, :, :]]
        win_scores = jnp.einsum('chd,icjhd->hcij', query_row, key_window) * scale_qk + offset_terms.transpose(0, 2, 1, 3)
        ctx_scores = jnp.einsum('chd,lhd->hcl', query_row, ctx_keys) * scale_qk
        logits = jnp.concatenate([win_scores.reshape(HEADS, GRID_W, WIN_H * WIN_W), ctx_scores], axis=-1)
        rounded = jax.nn.softmax(logits, axis=-1).astype(jnp.bfloat16)
        weights = lax.optimization_barrier(rounded).astype(jnp.float32)
        win_weights = weights[..., :WIN_H * WIN_W].reshape(HEADS, GRID_W, WIN_H, WIN_W)
        result = jnp.einsum('hcij,icjhd->chd', win_weights, value_window)
        result = result + jnp.einsum('hcl,lhd->chd', weights[..., WIN_H * WIN_W:], ctx_values)
        return result.astype(jnp.bfloat16)
    attended = lax.map(one_row, jnp.arange(grid_rows, dtype=jnp.int32))
    attended = attended.reshape(grid_rows * GRID_W, HEADS * HEAD_DIM)
    branch = jnp.dot(attended, w_out, preferred_element_type=jnp.float32)
    return (latent.astype(jnp.float32) + gate_vec * branch).astype(jnp.bfloat16)
```

```python
import functools

import jax
import jax.numpy as jnp
from jax import lax
from jax.experimental import pallas as pl
from jax.experimental.pallas import tpu as pltpu
from jax.sharding import PartitionSpec as P

HEAD_DIM = 64
GRID_W = 64
WIN_H = 8
WIN_W = 16
EPSILON = 1e-06
LANES = 128
BEFORE = WIN_H // 2
AFTER = WIN_H - BEFORE - 1
MESH = pl.DeviceIdType.MESH
F32 = jnp.float32
BF16 = jnp.bfloat16
NT = (((1,), (1,)), ((), ()))


def silu(v):
    v = v.astype(F32)
    return v / (1.0 + jnp.exp(-v))


def row_scales(rows_ref, start, inv_ref, at, step):
    width = rows_ref.shape[1]
    total = jnp.zeros((step, LANES), F32)
    for b in range(width // LANES):
        v = rows_ref[pl.ds(start, step), b * LANES : (b + 1) * LANES].astype(F32)
        total = total + v * v
    mean = jnp.sum(total, axis=1, keepdims=True) * (1.0 / width)
    inv_ref[pl.ds(at, step), :] = jnp.broadcast_to(lax.rsqrt(mean + EPSILON), (step, LANES))


def kernel(
    S, T,
    cond_ref, vec_ref, ctx_in, wsh_ref, wsc_ref, wga_ref, gain_ref, offs_ref,
    x_hbm, wq_hbm, wk_hbm, wv_hbm, wo_hbm,
    out_ref,
    x, w, wo, wl, wc, hb, ha, ctx, parts, mods, gate, offs, table, inv, inv_c,
    shf, shb, q_s, k_ext, v_ext, kc_s, vc_s, att,
    load_sem, ready, part_send, part_recv, ctx_send, ctx_recv, fwd_send, fwd_recv,
    halo_send, halo_recv, hb_send, hb_recv, ha_send, ha_recv, mod_send, mod_recv, att_send, att_recv,
):
    z = lax.axis_index("sp")
    t = lax.axis_index("tp")
    tokens, width = x.shape
    rows_dev = tokens // GRID_W
    cols = wsh_ref.shape[1]
    halves = cols // LANES
    rows_ctx = ctx_in.shape[0]
    slab = pl.ds(pl.multiple_of(t * cols, cols), cols)
    n_b, n_a = hb.shape[0], ha.shape[0]

    def peer(k):
        return lax.rem(t + k, T)

    def remote(src, dst, send, recv, **where):
        return pltpu.make_async_remote_copy(
            src_ref=src, dst_ref=dst, send_sem=send, recv_sem=recv,
            device_id=where, device_id_type=MESH,
        )

    barrier = pltpu.get_barrier_semaphore()
    for k in range(1, T):
        pl.semaphore_signal(barrier, inc=1, device_id={"tp": peer(k)}, device_id_type=MESH)

    def say_here(i, _):
        pl.semaphore_signal(barrier, inc=1, device_id={"sp": i}, device_id_type=MESH)
        return 0

    lax.fori_loop(z + 1, S, say_here, 0)

    loads = [
        pltpu.make_async_copy(x_hbm, x, load_sem.at[0]),
        pltpu.make_async_copy(wq_hbm, w.at[:, 0:LANES], load_sem.at[1]),
        pltpu.make_async_copy(wk_hbm, w.at[:, LANES : 2 * LANES], load_sem.at[2]),
        pltpu.make_async_copy(wv_hbm, w.at[:, 2 * LANES : 3 * LANES], load_sem.at[3]),
        pltpu.make_async_copy(wo_hbm, wo, load_sem.at[4]),
    ]
    for load in loads:
        load.start()

    row = lax.broadcasted_iota(jnp.int32, (16, cond_ref.shape[1]), 0)
    acts = jnp.where(row == 0, silu(cond_ref[...]), silu(vec_ref[...])).astype(BF16)
    shift_p = jnp.dot(acts, wsh_ref[...], preferred_element_type=F32)
    scale_p = jnp.dot(acts, wsc_ref[...], preferred_element_type=F32)
    gate_p = jnp.dot(acts, wga_ref[...], preferred_element_type=F32)
    for h in range(halves):
        lanes = slice(h * LANES, (h + 1) * LANES)
        parts[z, 2 * h : 2 * h + 2, :] = shift_p[0:2, lanes]
        parts[z, 4 + 2 * h : 6 + 2 * h, :] = scale_p[0:2, lanes]
        parts[z, 8 + h : 9 + h, :] = gate_p[0:1, lanes]
    ctx[pl.ds(pl.multiple_of(z * rows_ctx, rows_ctx), rows_ctx), :] = ctx_in[...]

    pl.semaphore_wait(barrier, z + (T - 1))

    def part_copy(src, to):
        return remote(parts.at[src], parts.at[src], part_send.at[to], part_recv.at[src], sp=to)

    def ctx_block(src):
        return ctx.at[pl.ds(pl.multiple_of(src * rows_ctx, rows_ctx), rows_ctx), slab]

    def ctx_copy(to):
        return remote(ctx_in.at[:, slab], ctx_block(z), ctx_send.at[to], ctx_recv.at[z], sp=to)

    def ctx_arrival(src):
        return remote(ctx_in.at[:, slab], ctx_block(src), ctx_send.at[src], ctx_recv.at[src], sp=src)

    def send_down(i, _):
        pl.semaphore_signal(ready.at[z], inc=1, device_id={"sp": i}, device_id_type=MESH)
        part_copy(z, i).start()
        return 0

    lax.fori_loop(0, z, send_down, 0)

    def send_down_ctx(i, _):
        ctx_copy(i).start()
        return 0

    lax.fori_loop(0, z, send_down_ctx, 0)

    loads[0].wait()
    below = lax.rem(z + (S - 1), S)
    above = lax.rem(z + 1, S)
    to_below = remote(x.at[0:n_a, slab], ha.at[:, slab], halo_send.at[0], halo_recv.at[0], sp=below)
    to_above = remote(x.at[tokens - n_b : tokens, slab], hb.at[:, slab], halo_send.at[1], halo_recv.at[1], sp=above)

    @pl.when(z > 0)
    def _():
        to_below.start()

    zeros_offs = jnp.zeros(offs.shape, F32)
    offs[...] = zeros_offs
    n_off = offs_ref.shape[1]
    for hd in range(2):
        offs[hd, 0:n_off, 0 : offs_ref.shape[2]] = offs_ref[hd]
    qc = lax.broadcasted_iota(jnp.int32, (GRID_W, LANES), 0)
    kcol = lax.rem(lax.broadcasted_iota(jnp.int32, (GRID_W, LANES), 1), GRID_W)
    c0 = jnp.clip(qc - WIN_W // 2, 0, GRID_W - WIN_W)
    inside = (kcol >= c0) & (kcol < c0 + WIN_W)
    for hd in range(2):
        here = offs[hd, 0:16, :]
        first = pltpu.roll(here, LANES - (WIN_W - 1), 1)
        second = pltpu.roll(here, GRID_W - (WIN_W - 1), 1)
        for o in range(n_off - 1):
            line = first[o : o + 1, :] + second[o + 1 : o + 2, :]
            spread = pltpu.roll(jnp.broadcast_to(line, (GRID_W, LANES)), 0, 1, stride=1, stride_axis=0)
            table[o, hd * GRID_W : (hd + 1) * GRID_W, :] = jnp.where(inside, spread, -jnp.inf)

    step = GRID_W

    def own_scales(i, _):
        at = pl.multiple_of(i * step, step)
        row_scales(x, at, inv, pl.multiple_of(n_b + at, step), step)
        return 0

    lax.fori_loop(0, tokens // step, own_scales, 0)
    shf[...] = jnp.zeros(shf.shape, F32)

    @pl.when(z == 0)
    def _():
        hb[...] = jnp.zeros(hb.shape, BF16)

    @pl.when(z == S - 1)
    def _():
        ha[...] = jnp.zeros(ha.shape, BF16)

    def spread_rows(ref, send, recv):
        for k in range(1, T):
            p = peer(k)
            remote(ref.at[:, slab], ref.at[:, slab], send.at[p], recv.at[t], tp=p).start()

    at_a, at_b = min(2, S - 1), min(4, S - 1)

    def one_source(i, _):
        src = lax.rem(z + i, S)

        @pl.when(src > z)
        def _():
            pl.semaphore_wait(ready.at[src], 1)
            part_copy(z, src).start()
            ctx_copy(src).start()

        @pl.when((i == 1) & (z < S - 1))
        def _():
            to_above.start()

        ctx_arrival(src).wait_recv()
        for k in range(1, T):
            p = peer(k)
            remote(ctx_block(src), ctx_block(src), fwd_send.at[p], fwd_recv.at[t], tp=p).start()

        @pl.when((i == at_a) & (z < S - 1))
        def _():
            to_below.wait_recv()
            spread_rows(ha, ha_send, ha_recv)

        @pl.when((i == at_b) & (z > 0))
        def _():
            to_above.wait_recv()
            spread_rows(hb, hb_send, hb_recv)

        return 0

    mid = max(S // 2, at_b + 1)
    lax.fori_loop(1, mid, one_source, 0)

    def slab_of(p):
        return pl.ds(pl.multiple_of(p * cols, cols), cols)

    def await_rows(ref, send, recv):
        for k in range(1, T):
            p = peer(k)
            remote(ref.at[:, slab_of(p)], ref.at[:, slab_of(p)], send.at[p], recv.at[p], tp=p).wait_recv()

    @pl.when(z < S - 1)
    def _():
        await_rows(ha, ha_send, ha_recv)

    @pl.when(z > 0)
    def _():
        await_rows(hb, hb_send, hb_recv)

    def before_scales(i, _):
        at = pl.multiple_of(i * step, step)
        row_scales(hb, at, inv, at, step)
        return 0

    def after_scales(i, _):
        at = pl.multiple_of(i * step, step)
        row_scales(ha, at, inv, pl.multiple_of(n_b + tokens + at, step), step)
        return 0

    lax.fori_loop(0, n_b // step, before_scales, 0)
    lax.fori_loop(0, n_a // step, after_scales, 0)
    for load in loads[1:]:
        load.wait()

    if mid < S:
        lax.fori_loop(mid, S, one_source, 0)

    def await_part(i, _):
        src = lax.rem(z + i, S)
        part_copy(src, src).wait_recv()
        return 0

    lax.fori_loop(1, S, await_part, 0)
    total = parts[0]
    for s in range(1, S):
        total = total + parts[s]
    mods[t] = total[0:8, :]
    gate[...] = total[8 : 8 + halves, :]
    for k in range(1, T):
        p = peer(k)
        remote(mods.at[t], mods.at[t], mod_send.at[p], mod_recv.at[t], tp=p).start()

    most = ctx.shape[0] - rows_ctx
    for k in range(1, T):
        p = peer(k)
        some = ctx.at[0:most, slab_of(p)]
        remote(some, some, fwd_send.at[p], fwd_recv.at[p], tp=p).wait_recv()
    c_step = min(step, ctx.shape[0])

    def ctx_scales(i, _):
        at = pl.multiple_of(i * c_step, c_step)
        row_scales(ctx, at, inv_c, at, c_step)
        return 0

    lax.fori_loop(0, ctx.shape[0] // c_step, ctx_scales, 0)

    for k in range(1, T):
        p = peer(k)
        remote(mods.at[p], mods.at[p], mod_send.at[p], mod_recv.at[p], tp=p).wait_recv()

    factors = []
    for h in range(halves):
        g = gain_ref[h].astype(F32)
        for m in range(2):
            factors.append((1.0 + mods[:, 4 + 2 * h + m, :]) * g)
    upright = jnp.concatenate(factors, axis=0).T
    for f in range(T):
        for h in range(halves):
            lo = (f * halves + h) * LANES
            block = w[lo : lo + LANES, :].astype(F32)
            at = 2 * h * T + f
            wl[lo : lo + LANES, :] = (block * upright[:, at : at + 1]).astype(BF16)
            at = (2 * h + 1) * T + f
            wc[lo : lo + LANES, :] = (block[:, LANES:] * upright[:, at : at + 1]).astype(BF16)
            shf[0:2, lo : lo + LANES] = mods[f, 2 * h : 2 * h + 2, :]
    shift = shf[...]
    high = shift.astype(BF16)
    shb[0:8, :] = high
    shb[8:16, :] = (shift - high.astype(F32)).astype(BF16)
    base = jnp.dot(shb[...], w[...], preferred_element_type=F32)
    base_l = base[0:1, :] + base[8:9, :]
    base_c = base[1:2, LANES:] + base[9:10, LANES:]

    def three(v):
        return jnp.concatenate([v, v, v], axis=1)

    def two(v):
        return jnp.concatenate([v, v], axis=1)

    own = jnp.dot(x[...], wl[...], preferred_element_type=F32)
    own = own * three(inv[n_b : n_b + tokens, :]) + base_l
    q_s[...] = (own[:, 0:LANES].astype(BF16).astype(F32) * HEAD_DIM ** (-0.5)).astype(BF16)
    k_ext[BEFORE : BEFORE + rows_dev] = own[:, LANES : 2 * LANES].astype(BF16).reshape(rows_dev, GRID_W, LANES)
    v_ext[BEFORE : BEFORE + rows_dev] = own[:, 2 * LANES :].astype(BF16).reshape(rows_dev, GRID_W, LANES)
    kv_b = jnp.dot(hb[...], wl[:, LANES:], preferred_element_type=F32) * two(inv[0:n_b, :]) + base_l[:, LANES:]
    k_ext[0:BEFORE] = kv_b[:, 0:LANES].astype(BF16).reshape(BEFORE, GRID_W, LANES)
    v_ext[0:BEFORE] = kv_b[:, LANES:].astype(BF16).reshape(BEFORE, GRID_W, LANES)
    kv_a = jnp.dot(ha[...], wl[:, LANES:], preferred_element_type=F32) * two(inv[n_b + tokens :, :]) + base_l[:, LANES:]
    k_ext[BEFORE + rows_dev :] = kv_a[:, 0:LANES].astype(BF16).reshape(AFTER, GRID_W, LANES)
    v_ext[BEFORE + rows_dev :] = kv_a[:, LANES:].astype(BF16).reshape(AFTER, GRID_W, LANES)
    kv_c = jnp.dot(ctx[...], wc[...], preferred_element_type=F32) * two(inv_c[...]) + base_c
    kc_s[...] = kv_c[:, 0:LANES].astype(BF16)
    vc_s[...] = kv_c[:, LANES:].astype(BF16)

    head0 = lax.broadcasted_iota(jnp.int32, (GRID_W, LANES), 1) < HEAD_DIM
    own_cols = pl.ds(pl.multiple_of(t * LANES, LANES), LANES)
    group = 2
    for r in range(rows_dev):
        grid_row = z * rows_dev + r
        first_row = jnp.clip(grid_row - WIN_H // 2, 0, S * rows_dev - WIN_H)
        start = first_row - z * rows_dev + BEFORE
        offset = first_row - grid_row + WIN_H - 1
        q = q_s[r * GRID_W : (r + 1) * GRID_W, :]
        none = jnp.zeros_like(q)
        q2 = jnp.concatenate([jnp.where(head0, q, none), jnp.where(head0, none, q)], axis=0)
        keys = k_ext[pl.ds(start, WIN_H)].reshape(WIN_H * GRID_W, LANES)
        values = v_ext[pl.ds(start, WIN_H)].reshape(WIN_H * GRID_W, LANES)
        s_win = lax.dot_general(q2, keys, NT, preferred_element_type=F32)
        s_win = s_win + jnp.concatenate([table[offset + 2 * j] for j in range(WIN_H // 2)], axis=1)
        s_ctx = lax.dot_general(q2, kc_s[...], NT, preferred_element_type=F32)
        top = jnp.maximum(jnp.max(s_win, axis=1, keepdims=True), jnp.max(s_ctx, axis=1, keepdims=True))
        e_win = jnp.exp(s_win - top)
        e_ctx = jnp.exp(s_ctx - top)
        norm = jnp.sum(e_win, axis=1, keepdims=True) + jnp.sum(e_ctx, axis=1, keepdims=True)
        o = jnp.dot(e_win.astype(BF16), values, preferred_element_type=F32)
        o = o + jnp.dot(e_ctx.astype(BF16), vc_s[...], preferred_element_type=F32)
        o = o / norm
        o = jnp.where(head0, o[0:GRID_W, :], o[GRID_W:, :])
        att[r * GRID_W : (r + 1) * GRID_W, own_cols] = o.astype(BF16)
        if r % group == group - 1:
            g = r // group
            rows = slice(g * group * GRID_W, (g + 1) * group * GRID_W)
            for k in range(1, T):
                p = peer(k)
                remote(att.at[rows, own_cols], att.at[rows, own_cols], att_send.at[p, g], att_recv.at[t, g], tp=p).start()

    for g in range(rows_dev // group):
        rows = slice(g * group * GRID_W, (g + 1) * group * GRID_W)
        for k in range(1, T):
            p = peer(k)
            theirs = pl.ds(pl.multiple_of(p * LANES, LANES), LANES)
            remote(att.at[rows, theirs], att.at[rows, theirs], att_send.at[p, g], att_recv.at[p, g], tp=p).wait_recv()
        branch = jnp.dot(att[rows, :], wo[...], preferred_element_type=F32)
        residual = x[rows, slab].astype(F32)
        for h in range(halves):
            lanes = slice(h * LANES, (h + 1) * LANES)
            out_ref[rows, lanes] = (residual[:, lanes] + gate[h : h + 1, :] * branch[:, lanes]).astype(BF16)

    def sent_parts(i, _):
        to = lax.rem(z + i, S)
        part_copy(z, to).wait_send()
        ctx_copy(to).wait_send()
        return 0

    lax.fori_loop(1, S, sent_parts, 0)

    @pl.when(z > 0)
    def _():
        to_below.wait_send()
        for k in range(1, T):
            p = peer(k)
            remote(hb.at[:, slab], hb.at[:, slab], hb_send.at[p], hb_recv.at[t], tp=p).wait_send()

    @pl.when(z < S - 1)
    def _():
        to_above.wait_send()
        for k in range(1, T):
            p = peer(k)
            remote(ha.at[:, slab], ha.at[:, slab], ha_send.at[p], ha_recv.at[t], tp=p).wait_send()

    for k in range(1, T):
        p = peer(k)
        some = ctx.at[0:most, slab]
        remote(some, some, fwd_send.at[p], fwd_recv.at[t], tp=p).wait_send()
        remote(mods.at[t], mods.at[t], mod_send.at[p], mod_recv.at[t], tp=p).wait_send()
        for g in range(rows_dev // group):
            rows = slice(g * group * GRID_W, (g + 1) * group * GRID_W)
            remote(att.at[rows, own_cols], att.at[rows, own_cols], att_send.at[p, g], att_recv.at[t, g], tp=p).wait_send()


def local(
    S, T, latent, conditioning, context, ctx_vector, w_shift, w_scale, w_gate, norm_gain,
    w_query, w_key, w_value, offset_bias, w_out,
):
    tokens, width = latent.shape
    cols = w_shift.shape[1]
    halves = cols // LANES
    rows_dev = tokens // GRID_W
    n_ctx = context.shape[0] * S
    ext = rows_dev + BEFORE + AFTER
    heads, n_off, _ = offset_bias.shape
    dma = pltpu.SemaphoreType.DMA
    vmem = pl.BlockSpec(memory_space=pltpu.VMEM)
    hbm = pl.BlockSpec(memory_space=pltpu.HBM)
    gain = norm_gain.reshape(T, halves, LANES).transpose(1, 0, 2)
    return pl.pallas_call(
        functools.partial(kernel, S, T),
        name="modulated_attention",
        out_shape=jax.ShapeDtypeStruct((tokens, cols), BF16),
        in_specs=[vmem] * 8 + [hbm] * 5,
        out_specs=vmem,
        scratch_shapes=[
            pltpu.VMEM((tokens, width), BF16),
            pltpu.VMEM((width, 3 * LANES), BF16),
            pltpu.VMEM(w_out.shape, BF16),
            pltpu.VMEM((width, 3 * LANES), BF16),
            pltpu.VMEM((width, 2 * LANES), BF16),
            pltpu.VMEM((BEFORE * GRID_W, width), BF16),
            pltpu.VMEM((AFTER * GRID_W, width), BF16),
            pltpu.VMEM((n_ctx, width), BF16),
            pltpu.VMEM((S, 8 + halves, LANES), F32),
            pltpu.VMEM((T, 8, LANES), F32),
            pltpu.VMEM((halves, LANES), F32),
            pltpu.VMEM((heads, 16, LANES), F32),
            pltpu.VMEM((n_off - 1, heads * GRID_W, LANES), F32),
            pltpu.VMEM((ext * GRID_W, LANES), F32),
            pltpu.VMEM((n_ctx, LANES), F32),
            pltpu.VMEM((8, width), F32),
            pltpu.VMEM((16, width), BF16),
            pltpu.VMEM((tokens, LANES), BF16),
            pltpu.VMEM((ext, GRID_W, LANES), BF16),
            pltpu.VMEM((ext, GRID_W, LANES), BF16),
            pltpu.VMEM((n_ctx, LANES), BF16),
            pltpu.VMEM((n_ctx, LANES), BF16),
            pltpu.VMEM((tokens, T * LANES), BF16),
            dma((5,)),
            pltpu.SemaphoreType.REGULAR((S,)),
            dma((S,)), dma((S,)), dma((S,)), dma((S,)),
            dma((T,)), dma((T,)),
            dma((2,)), dma((2,)),
            dma((T,)), dma((T,)), dma((T,)), dma((T,)),
            dma((T,)), dma((T,)),
            dma((T, rows_dev // 2)), dma((T, rows_dev // 2)),
        ],
        compiler_params=pltpu.CompilerParams(collective_id=0, has_side_effects=True),
    )(
        conditioning.reshape(1, -1), ctx_vector.reshape(1, -1), context, w_shift, w_scale, w_gate,
        gain, offset_bias, latent, w_query, w_key, w_value, w_out,
    )


def solution(mesh):
    return jax.shard_map(
        functools.partial(local, mesh.shape["sp"], mesh.shape["tp"]),
        mesh=mesh,
        in_specs=(
            P(("grp", "sp"), None),
            P(("grp", "sp")),
            P(("grp", "sp"), None),
            P("sp"),
            P("sp", "tp"),
            P("sp", "tp"),
            P("sp", "tp"),
            P(),
            P(None, "tp"),
            P(None, "tp"),
            P(None, "tp"),
            P("tp", None, None),
            P(None, "tp"),
        ),
        out_specs=P(("grp", "sp"), "tp"),
        check_vma=False,
    )
```
